32 devices in a mesh: tp: 8 (over z, y), dp: 4 (over x, core).
Axes of the slice: x: 2, y: 2, z: 4, core: 2. Of those that a mesh axis runs over, the one named last changes fastest.
Arguments:
- stream: bfloat16 [256, 2048], P('tp', 'dp'), may hold values from -12 to 12
- norm_gain: float32 [2, 2048], P(None, 'dp'), may hold values from 0.1 to 1.9
- w_input: bfloat16 [2, 2048, 2048], P(None, 'dp', 'tp'), may hold values from -0.125 to 0.125
- lam_re: float32 [2, 128, 64], P(None, 'tp'), may hold values from -1 to -0.05
- lam_im: float32 [2, 128, 64], P(None, 'tp'), may hold values from 0 to 6
- log_dt: float32 [2, 128], P(None, 'tp'), may hold values from -3 to 0
- b_re: float32 [2, 128, 64, 16], P(None, 'tp'), may hold values from -1 to 1
- b_im: float32 [2, 128, 64, 16], P(None, 'tp'), may hold values from -1 to 1
- readout_real: float32 [2, 128, 16, 64], P(None, 'tp'), may hold values from -0.5 to 0.5
- readout_imaginary: float32 [2, 128, 16, 64], P(None, 'tp'), may hold values from -0.5 to 0.5
- d_skip: float32 [2, 2048], P(None, 'tp'), may hold values from -4 to 4
- w_val: bfloat16 [2, 2048, 2048], P(None, 'tp', 'dp'), may hold values from -0.375 to 0.375
- w_gate: bfloat16 [2, 2048, 2048], P(None, 'tp', 'dp'), may hold values from -0.375 to 0.375
- state: float32 [2, 256, 128, 128], P(None, 'dp', 'tp'), may hold values from -6 to 6
Outputs:
- stream_out: bfloat16 [256, 2048], P('tp', 'dp')
- states_out: float32 [2, 256, 128, 128], P(None, 'dp', 'tp')
The draws below stay inside these ranges and needn't reach their ends.
All inputs are finite; a program needn't handle non-finite values.
Results may differ from the reference program's by a relative error of at most 0.0064.
Values may be sent and summed in bfloat16 or wider, within the bound.
A program may use at most 64 MiB of HBM per device.

```python
import jax
import jax.numpy as jnp
from jax import lax

D = 2048
CH = 16
STATE = 64
GROUPS = 128
LAYERS = 2
SEQS = 256


def draw_stream(key, part):
    subkeys = jax.random.split(key, 2)
    base_draw = jax.random.normal(subkeys[0], (SEQS, D), jnp.float32)
    block_scale = jnp.exp(jax.random.uniform(subkeys[1], (SEQS, 8), jnp.float32, -1.2, 1.2))
    full_draw = base_draw * jnp.repeat(block_scale, D // 8, axis=1)
    return jnp.clip(full_draw, -12.0, 12.0).astype(jnp.bfloat16)


def level_of(rng, extent, cuts, low, largest):
    loudness, own = 1.0, jax.random.fold_in(rng, 6)
    for dim, shards_of in cuts:
        heights = jnp.exp(jax.random.uniform(jax.random.fold_in(own, dim), (shards_of,), jnp.float32, low / len(cuts), largest / len(cuts)))
        loudness = loudness * jnp.repeat(heights, extent[dim] // shards_of).reshape([-1 if axis == dim else 1 for axis in range(len(extent))])
    return loudness


def bell_draw(rng, shape, scale, limit, cuts=(), held_as=jnp.bfloat16):
    result = scale * jax.random.normal(rng, shape, jnp.float32)
    if cuts:
        result = result * level_of(rng, shape, cuts, -0.22, 0.18)
    return jnp.clip(result, -limit, limit).astype(held_as)


def setup_inputs(seed: int = 0) -> dict:
    keys = jax.random.split(jax.random.key(seed), 15)
    stream = draw_stream(jax.random.fold_in(keys[14], 71), 0)
    norm_gain = jnp.clip(1.0 + 0.18 * jax.random.normal(keys[1], (LAYERS, D), jnp.float32), 0.1, 1.9)
    w_input = bell_draw(keys[2], (LAYERS, D, D), D ** -0.5, 0.125, ((1, 4), (2, 8)))
    lam_re = jnp.clip(-1.0 + 0.95 * jax.random.uniform(keys[3], (LAYERS, GROUPS, STATE), jnp.float32) ** level_of(keys[3], (LAYERS, GROUPS, STATE), ((1, 8),), -0.2, 0.2), -1.0, -0.05)
    lam_im = jnp.clip(6.0 * jax.random.uniform(keys[4], (LAYERS, GROUPS, STATE), jnp.float32) ** level_of(keys[4], (LAYERS, GROUPS, STATE), ((1, 8),), -0.2, 0.2), 0.0, 6.0)
    log_dt = jnp.clip(-3.0 + 3.0 * jax.random.uniform(keys[5], (LAYERS, GROUPS), jnp.float32) ** level_of(keys[5], (LAYERS, GROUPS), ((1, 8),), -0.2, 0.2), -3.0, 0.0)
    b_re = bell_draw(keys[6], (LAYERS, GROUPS, STATE, CH), (2 * CH) ** -0.5, 1.0, ((1, 8),), jnp.float32)
    b_im = bell_draw(keys[7], (LAYERS, GROUPS, STATE, CH), (2 * CH) ** -0.5, 1.0, ((1, 8),), jnp.float32)
    readout_real = bell_draw(keys[8], (LAYERS, GROUPS, CH, STATE), (2 * STATE) ** -0.5, 0.5, ((1, 8),), jnp.float32)
    readout_imaginary = bell_draw(keys[9], (LAYERS, GROUPS, CH, STATE), (2 * STATE) ** -0.5, 0.5, ((1, 8),), jnp.float32)
    d_skip = bell_draw(keys[10], (LAYERS, D), 1.0, 4.0, ((1, 8),), jnp.float32)
    w_val = bell_draw(keys[11], (LAYERS, D, D), (D // 8) ** -0.5, 0.375, ((1, 8), (2, 4)))
    w_gate = bell_draw(keys[12], (LAYERS, D, D), (D // 8) ** -0.5, 0.375, ((1, 8), (2, 4)))
    state = bell_draw(keys[13], (LAYERS, SEQS, GROUPS, 2 * STATE), 1.0, 6.0, ((1, 4), (2, 8)), jnp.float32)
    return {"stream": stream, "norm_gain": norm_gain, "w_input": w_input, "lam_re": lam_re, "lam_im": lam_im, "log_dt": log_dt, "b_re": b_re, "b_im": b_im, "readout_real": readout_real, "readout_imaginary": readout_imaginary, "d_skip": d_skip, "w_val": w_val, "w_gate": w_gate, "state": state}


eps = 1e-06

def advance(inputs, old_state, lam_re, lam_im, log_dt, b_re, b_im, readout_real, readout_imaginary, d_skip):
    upper_bound = lax.Precision.HIGHEST
    count_rows, groups, doubled = old_state.shape
    half_state = doubled // 2
    chans = b_re.shape[-1]
    step_size = jnp.exp(log_dt)[:, None]
    decay = jnp.exp(lam_re * step_size)
    angle = lam_im * step_size
    keep_re = decay * jnp.cos(angle)
    keep_im = decay * jnp.sin(angle)
    denom = lam_re * lam_re + lam_im * lam_im
    ratio_re = ((keep_re - 1.0) * lam_re + keep_im * lam_im) / denom
    ratio_im = (keep_im * lam_re - (keep_re - 1.0) * lam_im) / denom
    drive_re = ratio_re[..., None] * b_re - ratio_im[..., None] * b_im
    drive_im = ratio_re[..., None] * b_im + ratio_im[..., None] * b_re
    grouped = inputs.reshape(count_rows, groups, chans)
    push_re = jnp.einsum('gpc,rgc->rgp', drive_re, grouped, precision=upper_bound)
    push_im = jnp.einsum('gpc,rgc->rgp', drive_im, grouped, precision=upper_bound)
    old_re = old_state[..., :half_state]
    old_im = old_state[..., half_state:]
    updated_real = keep_re * old_re - keep_im * old_im + push_re
    updated_imaginary = keep_re * old_im + keep_im * old_re + push_im
    readout_output = jnp.einsum('aot,mat->mao', readout_real, updated_real, precision=upper_bound) - jnp.einsum('aot,mat->mao', readout_imaginary, updated_imaginary, precision=upper_bound)
    pre_act = readout_output.reshape(count_rows, groups * chans) + d_skip * inputs
    return (pre_act, jnp.concatenate([updated_real, updated_imaginary], axis=-1))

def reference(stream, norm_gain, w_input, lam_re, lam_im, log_dt, b_re, b_im, readout_real, readout_imaginary, d_skip, w_val, w_gate, state):
    collected = []
    for layer_no in range(LAYERS):
        widened = stream.astype(jnp.float32)
        factor = lax.rsqrt(lax.optimization_barrier(jnp.mean(widened * widened, axis=1)) + eps)
        normed = (widened * norm_gain[layer_no]).astype(jnp.bfloat16)
        inputs = factor[:, None] * jnp.dot(normed, w_input[layer_no], preferred_element_type=jnp.float32)
        pre_act, new_state = advance(inputs, state[layer_no], lam_re[layer_no], lam_im[layer_no], log_dt[layer_no], b_re[layer_no], b_im[layer_no], readout_real[layer_no], readout_imaginary[layer_no], d_skip[layer_no])
        mixed = jax.nn.gelu(pre_act).astype(jnp.bfloat16)
        value = jnp.dot(mixed, w_val[layer_no], preferred_element_type=jnp.float32)
        gate = jnp.dot(mixed, w_gate[layer_no], preferred_element_type=jnp.float32)
        stream = (widened + value * jax.nn.sigmoid(gate)).astype(jnp.bfloat16)
        collected.append(new_state)
    return (stream, jnp.stack(collected))
```

```python
import functools

import jax
import jax.numpy as jnp
from jax import lax
from jax.experimental import pallas as pl
from jax.experimental.pallas import tpu as pltpu
from jax.sharding import PartitionSpec as P

EPS = 1e-06
F32 = jnp.float32
BF16 = jnp.bfloat16
HIGHEST = lax.Precision.HIGHEST
NT = (((1,), (1,)), ((), ()))


def partner(me, k, n, back=False):
    if n & (n - 1):
        return (me + (n - k if back else k)) % n
    found, bit = 0, 1
    while bit < n:
        mine = (me // bit) % 2
        found = found + (bit * (1 - mine) if k & bit else bit * mine)
        bit *= 2
    return found


def kernel(
    tp, dp, chans,
    stream_ref, gain_ref, w_in_hbm, lam_re_ref, lam_im_ref, log_dt_ref, b_re_hbm, b_im_hbm, c_re_hbm, c_im_hbm, skip_ref,
    w_val_hbm, w_gate_hbm, state_hbm,
    out_ref, state,
    gains, w_in, w_wide, w_val, w_gate, b_re, b_im, c_re, c_im, drive, read,
    kept, proj, u_keep, masked, from_old, mix_w,
    x_own, x_all, x_wide, part_send, part_recv, sq_send, sq_recv, mix_all, block, comb_send, comb_own, pair_recv, comb_recv,
    load_sem, gain_ss, gain_rs, give_ss, give_rs, pass_ss, x_ss, x_rs, part_ss, part_rs, sq_ss, sq_rs, mix_ss, mix_rs, pair_ss, pair_rs, comb_ss, comb_rs,
):
    layers = b_re.shape[0]
    me_t, me_d = lax.axis_index("tp"), lax.axis_index("dp")
    rows_t, feats = stream_ref.shape
    rows_d, width = u_keep.shape[1:]
    per = rows_d // rows_t
    me_p, side = me_t // 2, me_t % 2
    groups, half = lam_re_ref.shape[1:]
    lanes = state.shape[2]
    sq_width = sq_send.shape[2]
    me_x, core, home = me_d // 2, me_d % 2, me_t // per
    mate = 2 * me_x + 1 - core

    loads = {}
    for l in range(layers):
        for i, (src, dst) in enumerate(
            (
                (b_re_hbm, b_re), (b_im_hbm, b_im), (c_re_hbm, c_re), (c_im_hbm, c_im), (state_hbm, state),
                (w_in_hbm, w_in), (w_val_hbm, w_val), (w_gate_hbm, w_gate),
            )
        ):
            to = dst.at[l] if i != 5 else w_wide.at[l - 1, me_d] if l else w_in
            loads[l, i] = pltpu.make_async_copy(src.at[l], to, load_sem.at[l, i])
            loads[l, i].start()

    barrier = pltpu.get_barrier_semaphore()
    for k in range(1, dp):
        pl.semaphore_signal(barrier, inc=1, device_id={"dp": partner(me_d, k, dp)}, device_id_type=pl.DeviceIdType.MESH)
    for k in range(1, tp):
        pl.semaphore_signal(barrier, inc=1, device_id={"tp": partner(me_t, k, tp)}, device_id_type=pl.DeviceIdType.MESH)

    def send(src, dst, ss, rs, axis, to):
        return pltpu.make_async_remote_copy(
            src_ref=src, dst_ref=dst, send_sem=ss, recv_sem=rs, device_id={axis: to}, device_id_type=pl.DeviceIdType.MESH
        )

    def x_copy(l, k):
        to = partner(me_t, k, tp)
        if l == 0:
            return send(stream_ref, x_all.at[me_t], x_ss.at[l, to], x_rs.at[l, me_t], "tp", to)
        slot = me_t % per
        return pltpu.make_async_remote_copy(
            src_ref=x_own.at[l - 1], dst_ref=x_wide.at[l - 1, me_d, slot], send_sem=x_ss.at[l, to],
            recv_sem=x_rs.at[l, me_d * per + slot], device_id={"tp": to, "dp": home}, device_id_type=pl.DeviceIdType.MESH,
        )

    def gain_copy(to):
        return send(gain_ref, gains.at[me_d], gain_ss.at[to], gain_rs.at[me_d], "dp", to)

    def give_copy(l, to):
        return send(w_in_hbm.at[l], w_wide.at[l - 1, me_d], give_ss.at[l - 1, to], give_rs.at[l - 1, me_d], "dp", to)

    def pass_copy(l, block):
        ref = w_wide.at[l - 1, block]
        return send(ref, ref, pass_ss.at[l - 1, block], give_rs.at[l - 1, block], "dp", mate)

    far = [2 * partner(me_x, k, dp // 2) + core for k in range(1, dp // 2)]

    def part_copy(to):
        return send(part_send.at[to], part_recv.at[me_d], part_ss.at[to], part_rs.at[me_d], "dp", to)

    def sq_copy(to):
        return send(sq_send.at[to], sq_recv.at[me_d], sq_ss.at[to], sq_rs.at[me_d], "dp", to)

    def mix_copy(l, to):
        return send(mix_all.at[l, me_d], mix_all.at[l, me_d], mix_ss.at[l, to], mix_rs.at[l, me_d], "dp", to)

    def comb_copy(l, to):
        return send(
            comb_send.at[l, 2 * to + side], comb_recv.at[l, me_p], comb_ss.at[l, to], comb_rs.at[l, me_p], "tp", 2 * to + side
        )

    def pair_copy(l, q):
        return send(
            comb_send.at[l, 2 * q + 1 - side], pair_recv.at[l, q], pair_ss.at[l, q], pair_rs.at[l, q], "tp", 2 * me_p + 1 - side
        )

    def arrival(ref, rs, axis):
        return send(ref, ref, rs, rs, axis, 0)

    lane_group = lax.broadcasted_iota(jnp.int32, (rows_d, width), 1) // chans
    eye = lax.broadcasted_iota(jnp.int32, (rows_d, sq_width), 0) == lax.broadcasted_iota(jnp.int32, (rows_d, sq_width), 1)

    group_eye = lax.broadcasted_iota(jnp.int32, (groups, groups), 0) == lax.broadcasted_iota(jnp.int32, (groups, groups), 1)

    def prepare(l):
        step_size = jnp.exp(jnp.sum(jnp.where(group_eye, log_dt_ref[l : l + 1, :], 0.0), axis=1, keepdims=True))
        lam_re, lam_im = lam_re_ref[l], lam_im_ref[l]
        decay = jnp.exp(lam_re * step_size)
        angle = lam_im * step_size
        keep_re = decay * jnp.cos(angle)
        keep_im = decay * jnp.sin(angle)
        denom = lam_re * lam_re + lam_im * lam_im
        ratio_re = ((keep_re - 1.0) * lam_re + keep_im * lam_im) / denom
        ratio_im = (keep_im * lam_re - (keep_re - 1.0) * lam_im) / denom
        keep_a = jnp.concatenate([keep_re, keep_re], axis=1)
        keep_b = jnp.concatenate([-keep_im, keep_im], axis=1)
        for i in range(5):
            loads[l, i].wait()
        for g in range(groups):
            t_re, t_im = b_re[l, g], b_im[l, g]
            r_re, r_im = ratio_re[g : g + 1, :], ratio_im[g : g + 1, :]
            drive[l, pl.ds(g * chans, chans), :] = jnp.concatenate(
                [r_re * t_re - r_im * t_im, r_re * t_im + r_im * t_re], axis=1
            )
        read[l] = jnp.concatenate([c_re[l].reshape(width, half), -c_im[l].reshape(width, half)], axis=1)
        for g in range(groups):
            old = state[l, pl.ds(g, rows_d, stride=groups), :]
            kept[l, pl.ds(g * rows_d, rows_d), :] = (
                keep_a[g : g + 1, :] * old + keep_b[g : g + 1, :] * pltpu.roll(old, lanes // 2, 1)
            )
        proj[...] = lax.dot_general(kept[l], read[l], NT, precision=HIGHEST, preferred_element_type=F32)
        total = jnp.zeros((rows_d, width), F32)
        for g in range(groups):
            total = jnp.where(lane_group == g, proj[pl.ds(g * rows_d, rows_d), :], total)
        from_old[l] = total
        full = lax.dot_general(drive[l], read[l], NT, precision=HIGHEST, preferred_element_type=F32)
        same = (
            lax.broadcasted_iota(jnp.int32, (width, width), 0) // chans
            == lax.broadcasted_iota(jnp.int32, (width, width), 1) // chans
        )
        mix_w[l] = jnp.where(same, full, 0.0)

    def update(l):
        u = u_keep[l]
        for g in range(groups):
            masked[pl.ds(g * rows_d, rows_d), :] = jnp.where(lane_group == g, u, 0.0)
        kept[l] = kept[l] + jnp.dot(masked[...], drive[l], precision=HIGHEST, preferred_element_type=F32)
        for g in range(groups):
            state[l, pl.ds(g, rows_d, stride=groups), :] = kept[l, pl.ds(g * rows_d, rows_d), :]

    pl.semaphore_wait(barrier, tp + dp - 2)
    for k in reversed(range(1, tp)):
        x_copy(0, k).start()
    for k in range(1, dp):
        gain_copy(partner(me_d, k, dp)).start()
    x_all[me_t] = stream_ref[...]
    gains[me_d] = gain_ref[...]
    prepare(0)

    for l in range(layers):
        loads[l, 5].wait()
        if l == 0:
            gain = gain_ref[l : l + 1, :]
            own_part = own_sq = None
            for k in reversed(range(dp)):
                to = partner(me_d, k, dp)
                for j in range(per):
                    t = to * per + j

                    @pl.when(t != me_t)
                    def _():
                        arrival(x_all.at[t], x_rs.at[l, t], "tp").wait_recv()

                x = x_all[pl.ds(to * per, per)].astype(F32).reshape(rows_d, feats)
                column = jnp.sum(x * x, axis=1, keepdims=True)
                squares = jnp.sum(jnp.where(eye, column, 0.0), axis=0, keepdims=True)
                product = jnp.dot((x * gain).astype(BF16), w_in[...], preferred_element_type=F32)
                if k:
                    sq_send[to] = jnp.broadcast_to(squares, (8, sq_width))
                    sq_copy(to).start()
                    part_send[to] = product.astype(BF16)
                    part_copy(to).start()
                else:
                    own_part, own_sq = product, squares
            for k in range(1, dp):
                by = partner(me_d, k, dp, True)
                arrival(sq_recv.at[by], sq_rs.at[by], "dp").wait_recv()
                own_sq = own_sq + sq_recv[by][0:1, :]
                arrival(part_recv.at[by], part_rs.at[by], "dp").wait_recv()
                own_part = own_part + part_recv[by].astype(F32)
            square_total = jnp.sum(jnp.where(eye, own_sq, 0.0), axis=1, keepdims=True)
        else:
            own_part = square_total = 0.0
            for k in range(dp):
                by = partner(me_d, k, dp, True)
                if k:
                    if l == 1:
                        arrival(gains.at[by], gain_rs.at[by], "dp").wait_recv()

                    @pl.when(by % 2 != core)
                    def _():
                        arrival(w_wide.at[l - 1, by], give_rs.at[l - 1, by], "dp").wait_recv()

                for j in range(per):

                    @pl.when((me_d * per + j != me_t) | (by != me_d))
                    def _():
                        arrival(x_wide.at[l - 1, by, j], x_rs.at[l, by * per + j], "tp").wait_recv()

                x = x_wide[l - 1, by].astype(F32).reshape(rows_d, feats)
                square_total = square_total + jnp.sum(x * x, axis=1, keepdims=True)
                normed = (x * gains[by, l : l + 1, :]).astype(BF16)
                own_part = own_part + jnp.dot(normed, w_wide[l - 1, by], preferred_element_type=F32)
        u = lax.rsqrt(square_total / (feats * dp) + EPS) * own_part
        u_keep[l] = u
        pre = from_old[l] + jnp.dot(u, mix_w[l], precision=HIGHEST, preferred_element_type=F32) + skip_ref[l : l + 1, :] * u
        mix_all[l, me_d] = jax.nn.gelu(pre).astype(BF16)
        for k in reversed(range(1, dp)):
            mix_copy(l, partner(me_d, k, dp)).start()
        if l + 1 < layers:
            for to in (*far, mate):
                give_copy(l + 1, to).start()
        loads[l, 6].wait()
        loads[l, 7].wait()

        def pass_on(by):
            for m in range(per // 2):
                q = by * (per // 2) + m
                arrival(pair_recv.at[l, q], pair_rs.at[l, q], "tp").wait_recv()
                total = block[2 * q + side] + pair_recv[l, q].astype(F32)

                @pl.when(q != me_p)
                def _():
                    comb_send[l, 2 * q + side] = total.astype(BF16)
                    comb_copy(l, q).start()

                @pl.when(q == me_p)
                def _():
                    comb_own[...] = total

        for k in range(dp):
            by = partner(me_d, k, dp, True)
            if k:
                arrival(mix_all.at[l, by], mix_rs.at[l, by], "dp").wait_recv()
            mixed = mix_all[l, by]
            value = jnp.dot(mixed, w_val[l], preferred_element_type=F32)
            gate = jnp.dot(mixed, w_gate[l], preferred_element_type=F32)
            for j in range(per):
                rows = slice(j * rows_t, (j + 1) * rows_t)
                block[by * per + j, :, :feats] = value[rows]
                block[by * per + j, :, feats:] = gate[rows]
            for m in range(per // 2):
                q = by * (per // 2) + m
                comb_send[l, 2 * q + 1 - side] = block[2 * q + 1 - side].astype(BF16)
                pair_copy(l, q).start()
            if k > 1:
                pass_on(partner(me_d, k - 2, dp, True))
        for k in range(max(dp - 2, 0), dp):
            pass_on(partner(me_d, k, dp, True))

        update(l)
        if l + 1 < layers:
            prepare(l + 1)
            for owner in far:
                arrival(w_wide.at[l, owner], give_rs.at[l, owner], "dp").wait_recv()
                pass_copy(l + 1, owner).start()
        combined = comb_own[...]
        for k in range(1, tp // 2):
            by = partner(me_p, k, tp // 2, True)
            arrival(comb_recv.at[l, by], comb_rs.at[l, by], "tp").wait_recv()
            combined = combined + comb_recv[l, by].astype(F32)
        old = x_own[l - 1] if l else stream_ref[...]
        fresh = (old.astype(F32) + combined[:, :feats] * jax.nn.sigmoid(combined[:, feats:])).astype(BF16)
        if l + 1 < layers:
            x_own[l] = fresh
            for k in reversed(range(1, tp)):
                x_copy(l + 1, k).start()
            pl.when(home != me_d)(lambda: x_copy(l + 1, 0).start())

            @pl.when(home == me_d)
            def _():
                x_wide[l, me_d, me_t % per] = fresh
        else:
            out_ref[...] = fresh

    for l in range(layers):
        for k in range(1, tp):
            x_copy(l, k).wait_send()
        if l:
            pl.when(home != me_d)(lambda: x_copy(l, 0).wait_send())
            for to in (*far, mate):
                give_copy(l, to).wait_send()
            for owner in far:
                pass_copy(l, owner).wait_send()
        for k in range(1, tp // 2):
            comb_copy(l, partner(me_p, k, tp // 2)).wait_send()
        for q in range(tp // 2):
            pair_copy(l, q).wait_send()
        for k in range(1, dp):
            mix_copy(l, partner(me_d, k, dp)).wait_send()
    for k in range(1, dp):
        to = partner(me_d, k, dp)
        gain_copy(to).wait_send()
        part_copy(to).wait_send()
        sq_copy(to).wait_send()


def store(x_ref, state_ref, x_out, state_out, sem):
    middle = state_ref.shape[0] // 2
    first, second = pl.ds(0, middle), pl.ds(middle, state_ref.shape[0] - middle)
    copies = [
        pltpu.make_async_copy(state_ref.at[first], state_out.at[first], sem.at[0]),
        pltpu.make_async_copy(state_ref.at[second], state_out.at[second], sem.at[1]),
        pltpu.make_async_copy(x_ref, x_out, sem.at[2]),
    ]
    for copy in copies:
        copy.start()
    for copy in copies:
        copy.wait()


def per_device(
    tp, dp,
    stream, norm_gain, w_input, lam_re, lam_im, log_dt, b_re, b_im, readout_real, readout_imaginary, d_skip,
    w_val, w_gate, state,
):
    layers, feats, width = w_input.shape
    rows_t = stream.shape[0]
    rows_d, groups, lanes = state.shape[1:]
    chans = b_re.shape[-1]

    turned_re, turned_im = b_re.swapaxes(2, 3), b_im.swapaxes(2, 3)

    limit = 67043328 - 4 * layers * rows_d * groups * lanes - (256 << 10)
    vmem = pl.BlockSpec(memory_space=pltpu.VMEM)
    hbm = pl.BlockSpec(memory_space=pltpu.HBM)
    sq_width = max(rows_d, 128)
    dma = lambda *shape: pltpu.SemaphoreType.DMA(shape)
    out, states = pl.pallas_call(
        functools.partial(kernel, tp, dp, chans),
        out_shape=(pltpu.VMEM(stream.shape, BF16), pltpu.VMEM((layers, rows_d * groups, lanes), F32)),
        in_specs=[vmem, vmem, hbm, vmem, vmem, vmem, hbm, hbm, hbm, hbm, vmem, hbm, hbm, hbm],
        out_specs=(vmem, vmem),
        scratch_shapes=[
            pltpu.VMEM((dp, layers, feats), F32),
            pltpu.VMEM((feats, width), BF16),
            pltpu.VMEM((layers - 1, dp, feats, width), BF16),
            pltpu.VMEM(w_val.shape, BF16),
            pltpu.VMEM(w_gate.shape, BF16),
            pltpu.VMEM(turned_re.shape, F32),
            pltpu.VMEM(turned_im.shape, F32),
            pltpu.VMEM(readout_real.shape, F32),
            pltpu.VMEM(readout_imaginary.shape, F32),
            pltpu.VMEM((layers, width, lanes), F32),
            pltpu.VMEM((layers, width, lanes), F32),
            pltpu.VMEM((layers, rows_d * groups, lanes), F32),
            pltpu.VMEM((rows_d * groups, width), F32),
            pltpu.VMEM((layers, rows_d, width), F32),
            pltpu.VMEM((rows_d * groups, width), F32),
            pltpu.VMEM((layers, rows_d, width), F32),
            pltpu.VMEM((layers, width, width), F32),
            pltpu.VMEM((layers - 1, rows_t, feats), BF16),
            pltpu.VMEM((tp, rows_t, feats), BF16),
            pltpu.VMEM((layers - 1, dp, rows_d // rows_t, rows_t, feats), BF16),
            pltpu.VMEM((dp, rows_d, width), BF16),
            pltpu.VMEM((dp, rows_d, width), BF16),
            pltpu.VMEM((dp, 8, sq_width), F32),
            pltpu.VMEM((dp, 8, sq_width), F32),
            pltpu.VMEM((layers, dp, rows_d, width), BF16),
            pltpu.VMEM((tp, rows_t, 2 * feats), F32),
            pltpu.VMEM((layers, tp, rows_t, 2 * feats), BF16),
            pltpu.VMEM((rows_t, 2 * feats), F32),
            pltpu.VMEM((layers, tp // 2, rows_t, 2 * feats), BF16),
            pltpu.VMEM((layers, tp // 2, rows_t, 2 * feats), BF16),
            dma(layers, 8),
            dma(dp), dma(dp),
            dma(layers - 1, dp), dma(layers - 1, dp), dma(layers - 1, dp),
            dma(layers, tp), dma(layers, tp),
            dma(dp), dma(dp),
            dma(dp), dma(dp),
            dma(layers, dp), dma(layers, dp),
            dma(layers, tp // 2), dma(layers, tp // 2),
            dma(layers, tp // 2), dma(layers, tp // 2),
        ],
        compiler_params=pltpu.CompilerParams(collective_id=0, has_side_effects=True, vmem_limit_bytes=limit),
    )(
        stream, norm_gain, w_input, lam_re, lam_im, log_dt, turned_re, turned_im, readout_real,
        readout_imaginary, d_skip, w_val, w_gate,
        state.reshape(layers, rows_d * groups, lanes),
    )
    hbm_out = lambda a: jax.ShapeDtypeStruct(a.shape, a.dtype)
    out, states = pl.pallas_call(
        store,
        out_shape=(hbm_out(stream), jax.ShapeDtypeStruct((layers, rows_d * groups, lanes), F32)),
        in_specs=[vmem, vmem],
        out_specs=(hbm, hbm),
        scratch_shapes=[dma(3)],
    )(*(pltpu.with_memory_space_constraint(a, pltpu.VMEM) for a in (out, states)))
    return out, states.reshape(state.shape)


def solution(mesh):
    return jax.shard_map(
        functools.partial(per_device, mesh.shape["tp"], mesh.shape["dp"]),
        mesh=mesh,
        in_specs=(
            P("tp", "dp"),
            P(None, "dp"),
            P(None, "dp", "tp"),
            P(None, "tp", None),
            P(None, "tp", None),
            P(None, "tp"),
            P(None, "tp", None, None),
            P(None, "tp", None, None),
            P(None, "tp", None, None),
            P(None, "tp", None, None),
            P(None, "tp"),
            P(None, "tp", "dp"),
            P(None, "tp", "dp"),
            P(None, "dp", "tp", None),
        ),
        out_specs=(P("tp", "dp"), P(None, "dp", "tp", None)),
        check_vma=False,
    )
```

```python
import functools

import jax
import jax.numpy as jnp
from jax import lax
from jax.experimental import pallas as pl
from jax.experimental.pallas import tpu as pltpu
from jax.sharding import PartitionSpec as P

EPS = 1e-06
F32 = jnp.float32
BF16 = jnp.bfloat16
HIGHEST = lax.Precision.HIGHEST
NT = (((1,), (1,)), ((), ()))


def partner(me, k, n, back=False):
    if n & (n - 1):
        return (me + (n - k if back else k)) % n
    found, bit = 0, 1
    while bit < n:
        mine = (me // bit) % 2
        found = found + (bit * (1 - mine) if k & bit else bit * mine)
        bit *= 2
    return found


def kernel(
    tp, dp, chans,
    stream_hbm, gain_hbm, w_in_hbm, lam_re_hbm, lam_im_hbm, log_dt_hbm, b_re_hbm, b_im_hbm, c_re_hbm, c_im_hbm, skip_hbm,
    w_val_hbm, w_gate_hbm, state_hbm,
    out_ref, state,
    stream_ref, gain_ref, lam_re_ref, lam_im_ref, log_dt_ref, skip_ref,
    gains, w_in, w_wide, w_val, w_gate, b_re, b_im, c_re, c_im, drive, read,
    kept, proj, u_keep, masked, from_old, mix_w,
    x_own, x_all, x_wide, x_rest, part_send, part_recv, sq_send, sq_recv, mix_all, block, comb_send, comb_own, pair_recv, comb_recv,
    small_sem, load_sem, gain_ss, gain_rs, give_ss, give_rs, pass_ss, rest_ss, rest_rs, x_ss, x_rs, part_ss, part_rs, sq_ss, sq_rs, mix_ss, mix_rs, pair_ss, pair_rs, comb_ss, comb_rs,
):
    layers = b_re.shape[0]
    me_t, me_d = lax.axis_index("tp"), lax.axis_index("dp")
    rows_t, feats = stream_ref.shape
    rows_d, width = u_keep.shape[1:]
    per = rows_d // rows_t
    me_p, side = me_t // 2, me_t % 2
    groups, half = lam_re_ref.shape[1:]
    lanes = state.shape[2]
    sq_width = sq_send.shape[2]
    me_x, core, home = me_d // 2, me_d % 2, me_t // per
    mate = 2 * me_x + 1 - core
    halves, pairs = dp // 2, per // 2
    spread = lambda block: block % 2 * halves + block // 2
    held = home % halves * 2 + home // halves
    final = held * per + me_t % per

    barrier = pltpu.get_barrier_semaphore()
    for k in range(1, dp):
        pl.semaphore_signal(barrier, inc=1, device_id={"dp": partner(me_d, k, dp)}, device_id_type=pl.DeviceIdType.MESH)
    for k in range(1, tp):
        pl.semaphore_signal(barrier, inc=1, device_id={"tp": partner(me_t, k, tp)}, device_id_type=pl.DeviceIdType.MESH)

    small = [
        pltpu.make_async_copy(src, dst, small_sem.at[i])
        for i, (src, dst) in enumerate(
            (
                (stream_hbm, stream_ref), (gain_hbm, gain_ref), (lam_re_hbm, lam_re_ref), (lam_im_hbm, lam_im_ref),
                (log_dt_hbm, log_dt_ref), (skip_hbm, skip_ref),
            )
        )
    ]
    for copy in small:
        copy.start()
    loads = {}
    for l in range(layers):
        for i, (src, dst) in enumerate(
            (
                (b_re_hbm, b_re), (b_im_hbm, b_im), (c_re_hbm, c_re), (c_im_hbm, c_im), (state_hbm, state),
                (w_in_hbm, w_in), (w_val_hbm, w_val), (w_gate_hbm, w_gate),
            )
        ):
            to = dst.at[l] if i != 5 else w_wide.at[l - 1, me_d] if l else w_in
            loads[l, i] = pltpu.make_async_copy(src.at[l], to, load_sem.at[l, i])
            loads[l, i].start()

    def send(src, dst, ss, rs, axis, to):
        return pltpu.make_async_remote_copy(
            src_ref=src, dst_ref=dst, send_sem=ss, recv_sem=rs, device_id={axis: to}, device_id_type=pl.DeviceIdType.MESH
        )

    def x_copy(l, k):
        to = partner(me_t, k, tp)
        if l == 0:
            return send(stream_ref, x_all.at[me_t], x_ss.at[l, to], x_rs.at[l, me_t], "tp", to)
        slot = me_t % per
        return pltpu.make_async_remote_copy(
            src_ref=x_own.at[l - 1], dst_ref=x_wide.at[l - 1, me_d, slot], send_sem=x_ss.at[l, to],
            recv_sem=x_rs.at[l, me_d * per + slot], device_id={"tp": to, "dp": held}, device_id_type=pl.DeviceIdType.MESH,
        )

    def rest_copy():
        return send(x_own.at[layers - 2], x_rest, rest_ss.at[0], rest_rs.at[0], "tp", final)

    def gain_copy(to):
        return send(gain_ref, gains.at[me_d], gain_ss.at[to], gain_rs.at[me_d], "dp", to)

    def give_copy(l, to):
        return send(w_in_hbm.at[l], w_wide.at[l - 1, me_d], give_ss.at[l - 1, to], give_rs.at[l - 1, me_d], "dp", to)

    def pass_copy(l, block):
        ref = w_wide.at[l - 1, block]
        return send(ref, ref, pass_ss.at[l - 1, block], give_rs.at[l - 1, block], "dp", mate)

    far = [2 * partner(me_x, k, dp // 2) + core for k in range(1, dp // 2)]

    def part_copy(to):
        return send(part_send.at[to], part_recv.at[me_d], part_ss.at[to], part_rs.at[me_d], "dp", to)

    def sq_copy(to):
        return send(sq_send.at[to], sq_recv.at[me_d], sq_ss.at[to], sq_rs.at[me_d], "dp", to)

    def mix_copy(l, to):
        return send(mix_all.at[l, me_d], mix_all.at[l, me_d], mix_ss.at[l, to], mix_rs.at[l, me_d], "dp", to)

    def comb_copy(l, r, to):
        return send(
            comb_send.at[l, 2 * r + side], comb_recv.at[l, me_p], comb_ss.at[l, to], comb_rs.at[l, me_p], "tp", 2 * to + side
        )

    def pair_copy(l, r):
        return send(
            comb_send.at[l, 2 * r + 1 - side], pair_recv.at[l, r], pair_ss.at[l, r], pair_rs.at[l, r], "tp", 2 * me_p + 1 - side
        )

    def arrival(ref, rs, axis):
        return send(ref, ref, rs, rs, axis, 0)

    lane_group = lax.broadcasted_iota(jnp.int32, (rows_d, width), 1) // chans
    eye = lax.broadcasted_iota(jnp.int32, (rows_d, sq_width), 0) == lax.broadcasted_iota(jnp.int32, (rows_d, sq_width), 1)

    group_eye = lax.broadcasted_iota(jnp.int32, (groups, groups), 0) == lax.broadcasted_iota(jnp.int32, (groups, groups), 1)

    def prepare(l):
        step_size = jnp.exp(jnp.sum(jnp.where(group_eye, log_dt_ref[l : l + 1, :], 0.0), axis=1, keepdims=True))
        lam_re, lam_im = lam_re_ref[l], lam_im_ref[l]
        decay = jnp.exp(lam_re * step_size)
        angle = lam_im * step_size
        keep_re = decay * jnp.cos(angle)
        keep_im = decay * jnp.sin(angle)
        denom = lam_re * lam_re + lam_im * lam_im
        ratio_re = ((keep_re - 1.0) * lam_re + keep_im * lam_im) / denom
        ratio_im = (keep_im * lam_re - (keep_re - 1.0) * lam_im) / denom
        keep_a = jnp.concatenate([keep_re, keep_re], axis=1)
        keep_b = jnp.concatenate([-keep_im, keep_im], axis=1)
        for i in range(5):
            loads[l, i].wait()
        for g in range(groups):
            t_re, t_im = b_re[l, g], b_im[l, g]
            r_re, r_im = ratio_re[g : g + 1, :], ratio_im[g : g + 1, :]
            drive[l, pl.ds(g * chans, chans), :] = jnp.concatenate(
                [r_re * t_re - r_im * t_im, r_re * t_im + r_im * t_re], axis=1
            )
        read[l] = jnp.concatenate([c_re[l].reshape(width, half), -c_im[l].reshape(width, half)], axis=1)
        for g in range(groups):
            old = state[l, pl.ds(g, rows_d, stride=groups), :]
            kept[l, pl.ds(g * rows_d, rows_d), :] = (
                keep_a[g : g + 1, :] * old + keep_b[g : g + 1, :] * pltpu.roll(old, lanes // 2, 1)
            )
        proj[...] = lax.dot_general(kept[l], read[l], NT, precision=HIGHEST, preferred_element_type=F32)
        total = jnp.zeros((rows_d, width), F32)
        for g in range(groups):
            total = jnp.where(lane_group == g, proj[pl.ds(g * rows_d, rows_d), :], total)
        from_old[l] = total
        full = lax.dot_general(drive[l], read[l], NT, precision=HIGHEST, preferred_element_type=F32)
        same = (
            lax.broadcasted_iota(jnp.int32, (width, width), 0) // chans
            == lax.broadcasted_iota(jnp.int32, (width, width), 1) // chans
        )
        mix_w[l] = jnp.where(same, full, 0.0)

    def update(l):
        u = u_keep[l]
        for g in range(groups):
            masked[pl.ds(g * rows_d, rows_d), :] = jnp.where(lane_group == g, u, 0.0)
        kept[l] = kept[l] + jnp.dot(masked[...], drive[l], precision=HIGHEST, preferred_element_type=F32)
        for g in range(groups):
            state[l, pl.ds(g, rows_d, stride=groups), :] = kept[l, pl.ds(g * rows_d, rows_d), :]

    small[0].wait()
    small[1].wait()
    pl.semaphore_wait(barrier, tp + dp - 2)
    for k in reversed(range(1, tp)):
        x_copy(0, k).start()
    for k in range(1, dp):
        gain_copy(partner(me_d, k, dp)).start()
    x_all[me_t] = stream_ref[...]
    gains[me_d] = gain_ref[...]
    for copy in small[2:]:
        copy.wait()
    prepare(0)

    for l in range(layers):
        loads[l, 5].wait()
        if l == 0:
            gain = gain_ref[l : l + 1, :]
            own_part = own_sq = None
            for k in reversed(range(dp)):
                to = partner(me_d, k, dp)
                for j in range(per):
                    t = to * per + j

                    @pl.when(t != me_t)
                    def _():
                        arrival(x_all.at[t], x_rs.at[l, t], "tp").wait_recv()

                x = x_all[pl.ds(to * per, per)].astype(F32).reshape(rows_d, feats)
                column = jnp.sum(x * x, axis=1, keepdims=True)
                squares = jnp.sum(jnp.where(eye, column, 0.0), axis=0, keepdims=True)
                product = jnp.dot((x * gain).astype(BF16), w_in[...], preferred_element_type=F32)
                if k:
                    sq_send[to] = jnp.broadcast_to(squares, (8, sq_width))
                    sq_copy(to).start()
                    part_send[to] = product.astype(BF16)
                    part_copy(to).start()
                else:
                    own_part, own_sq = product, squares
            for k in range(1, dp):
                by = partner(me_d, k, dp, True)
                arrival(sq_recv.at[by], sq_rs.at[by], "dp").wait_recv()
                own_sq = own_sq + sq_recv[by][0:1, :]
                arrival(part_recv.at[by], part_rs.at[by], "dp").wait_recv()
                own_part = own_part + part_recv[by].astype(F32)
            square_total = jnp.sum(jnp.where(eye, own_sq, 0.0), axis=1, keepdims=True)
        else:
            own_part = square_total = 0.0
            for k in range(dp):
                by = partner(me_d, k, dp, True)
                if k:
                    if l == 1:
                        arrival(gains.at[by], gain_rs.at[by], "dp").wait_recv()

                    @pl.when(by % 2 != core)
                    def _():
                        arrival(w_wide.at[l - 1, by], give_rs.at[l - 1, by], "dp").wait_recv()

                for j in range(per):

                    @pl.when((spread(me_d) * per + j != me_t) | (by != me_d))
                    def _():
                        arrival(x_wide.at[l - 1, by, j], x_rs.at[l, by * per + j], "tp").wait_recv()

                x = x_wide[l - 1, by].astype(F32).reshape(rows_d, feats)
                square_total = square_total + jnp.sum(x * x, axis=1, keepdims=True)
                normed = (x * gains[by, l : l + 1, :]).astype(BF16)
                own_part = own_part + jnp.dot(normed, w_wide[l - 1, by], preferred_element_type=F32)
        u = lax.rsqrt(square_total / (feats * dp) + EPS) * own_part
        u_keep[l] = u
        pre = from_old[l] + jnp.dot(u, mix_w[l], precision=HIGHEST, preferred_element_type=F32) + skip_ref[l : l + 1, :] * u
        mix_all[l, me_d] = jax.nn.gelu(pre).astype(BF16)
        for k in reversed(range(1, dp)):
            mix_copy(l, partner(me_d, k, dp)).start()
        if l + 1 < layers:
            for to in (*far, mate):
                give_copy(l + 1, to).start()
        loads[l, 6].wait()
        loads[l, 7].wait()

        def pass_on(by):
            for m in range(pairs):
                r = by * pairs + m
                q = (spread(by) if l + 1 < layers else by) * pairs + m
                arrival(pair_recv.at[l, r], pair_rs.at[l, r], "tp").wait_recv()
                total = block[2 * r + side] + pair_recv[l, r].astype(F32)

                @pl.when(q != me_p)
                def _():
                    comb_send[l, 2 * r + side] = total.astype(BF16)
                    comb_copy(l, r, q).start()

                @pl.when(q == me_p)
                def _():
                    comb_own[...] = total

        for k in range(dp):
            by = partner(me_d, k, dp, True)
            if k:
                arrival(mix_all.at[l, by], mix_rs.at[l, by], "dp").wait_recv()
            mixed = mix_all[l, by]
            value = jnp.dot(mixed, w_val[l], preferred_element_type=F32)
            gate = jnp.dot(mixed, w_gate[l], preferred_element_type=F32)
            for j in range(per):
                rows = slice(j * rows_t, (j + 1) * rows_t)
                block[by * per + j, :, :feats] = value[rows]
                block[by * per + j, :, feats:] = gate[rows]
            for m in range(pairs):
                r = by * pairs + m
                comb_send[l, 2 * r + 1 - side] = block[2 * r + 1 - side].astype(BF16)
                pair_copy(l, r).start()
            if k > 1:
                pass_on(partner(me_d, k - 2, dp, True))
        for k in range(max(dp - 2, 0), dp):
            pass_on(partner(me_d, k, dp, True))

        if l + 1 == layers:
            update(l)
        if l + 1 < layers:
            prepare(l + 1)
            for owner in far:
                arrival(w_wide.at[l, owner], give_rs.at[l, owner], "dp").wait_recv()
                pass_copy(l + 1, owner).start()
        combined = comb_own[...]
        for k in range(1, tp // 2):
            by = partner(me_p, k, tp // 2, True)
            arrival(comb_recv.at[l, by], comb_rs.at[l, by], "tp").wait_recv()
            combined = combined + comb_recv[l, by].astype(F32)
        if l == 0:
            old = x_all[final]
        elif l + 1 < layers:
            old = x_own[l - 1]
        else:
            pl.when(held != home)(lambda: arrival(x_rest, rest_rs.at[0], "tp").wait_recv())
            old = x_rest[...]
        fresh = (old.astype(F32) + combined[:, :feats] * jax.nn.sigmoid(combined[:, feats:])).astype(BF16)
        if l + 1 < layers:
            x_own[l] = fresh
            for k in reversed(range(1, tp)):
                x_copy(l + 1, k).start()
            pl.when(held != me_d)(lambda: x_copy(l + 1, 0).start())

            @pl.when(held == me_d)
            def _():
                x_wide[l, me_d, me_t % per] = fresh

            if l + 2 == layers:
                pl.when(held != home)(lambda: rest_copy().start())

                @pl.when(held == home)
                def _():
                    x_rest[...] = fresh

            update(l)
        else:
            out_ref[...] = fresh

    for l in range(layers):
        for k in range(1, tp):
            x_copy(l, k).wait_send()
        if l:
            pl.when(held != me_d)(lambda: x_copy(l, 0).wait_send())
            for to in (*far, mate):
                give_copy(l, to).wait_send()
            for owner in far:
                pass_copy(l, owner).wait_send()
        for k in range(1, tp // 2):
            comb_copy(l, 0, partner(me_p, k, tp // 2)).wait_send()
        for q in range(tp // 2):
            pair_copy(l, q).wait_send()
        for k in range(1, dp):
            mix_copy(l, partner(me_d, k, dp)).wait_send()
    pl.when(held != home)(lambda: rest_copy().wait_send())
    for k in range(1, dp):
        to = partner(me_d, k, dp)
        gain_copy(to).wait_send()
        part_copy(to).wait_send()
        sq_copy(to).wait_send()


def store(x_ref, state_ref, x_out, state_out, sem):
    middle = state_ref.shape[0] // 2
    first, second = pl.ds(0, middle), pl.ds(middle, state_ref.shape[0] - middle)
    copies = [
        pltpu.make_async_copy(state_ref.at[first], state_out.at[first], sem.at[0]),
        pltpu.make_async_copy(state_ref.at[second], state_out.at[second], sem.at[1]),
        pltpu.make_async_copy(x_ref, x_out, sem.at[2]),
    ]
    for copy in copies:
        copy.start()
    for copy in copies:
        copy.wait()


def per_device(
    tp, dp,
    stream, norm_gain, w_input, lam_re, lam_im, log_dt, b_re, b_im, readout_real, readout_imaginary, d_skip,
    w_val, w_gate, state,
):
    layers, feats, width = w_input.shape
    rows_t = stream.shape[0]
    rows_d, groups, lanes = state.shape[1:]
    chans = b_re.shape[-1]

    turned_re, turned_im = b_re.swapaxes(2, 3), b_im.swapaxes(2, 3)

    limit = 67043328 - 4 * layers * rows_d * groups * lanes - (256 << 10)
    vmem = pl.BlockSpec(memory_space=pltpu.VMEM)
    hbm = pl.BlockSpec(memory_space=pltpu.HBM)
    sq_width = max(rows_d, 128)
    dma = lambda *shape: pltpu.SemaphoreType.DMA(shape)
    out, states = pl.pallas_call(
        functools.partial(kernel, tp, dp, chans),
        out_shape=(pltpu.VMEM(stream.shape, BF16), pltpu.VMEM((layers, rows_d * groups, lanes), F32)),
        in_specs=[hbm] * 14,
        out_specs=(vmem, vmem),
        scratch_shapes=[
            pltpu.VMEM(stream.shape, BF16),
            *(pltpu.VMEM(a.shape, F32) for a in (norm_gain, lam_re, lam_im, log_dt, d_skip)),
            pltpu.VMEM((dp, layers, feats), F32),
            pltpu.VMEM((feats, width), BF16),
            pltpu.VMEM((layers - 1, dp, feats, width), BF16),
            pltpu.VMEM(w_val.shape, BF16),
            pltpu.VMEM(w_gate.shape, BF16),
            pltpu.VMEM(turned_re.shape, F32),
            pltpu.VMEM(turned_im.shape, F32),
            pltpu.VMEM(readout_real.shape, F32),
            pltpu.VMEM(readout_imaginary.shape, F32),
            pltpu.VMEM((layers, width, lanes), F32),
            pltpu.VMEM((layers, width, lanes), F32),
            pltpu.VMEM((layers, rows_d * groups, lanes), F32),
            pltpu.VMEM((rows_d * groups, width), F32),
            pltpu.VMEM((layers, rows_d, width), F32),
            pltpu.VMEM((rows_d * groups, width), F32),
            pltpu.VMEM((layers, rows_d, width), F32),
            pltpu.VMEM((layers, width, width), F32),
            pltpu.VMEM((layers - 1, rows_t, feats), BF16),
            pltpu.VMEM((tp, rows_t, feats), BF16),
            pltpu.VMEM((layers - 1, dp, rows_d // rows_t, rows_t, feats), BF16),
            pltpu.VMEM(stream.shape, BF16),
            pltpu.VMEM((dp, rows_d, width), BF16),
            pltpu.VMEM((dp, rows_d, width), BF16),
            pltpu.VMEM((dp, 8, sq_width), F32),
            pltpu.VMEM((dp, 8, sq_width), F32),
            pltpu.VMEM((layers, dp, rows_d, width), BF16),
            pltpu.VMEM((tp, rows_t, 2 * feats), F32),
            pltpu.VMEM((layers, tp, rows_t, 2 * feats), BF16),
            pltpu.VMEM((rows_t, 2 * feats), F32),
            pltpu.VMEM((layers, tp // 2, rows_t, 2 * feats), BF16),
            pltpu.VMEM((layers, tp // 2, rows_t, 2 * feats), BF16),
            dma(6),
            dma(layers, 8),
            dma(dp), dma(dp),
            dma(layers - 1, dp), dma(layers - 1, dp), dma(layers - 1, dp),
            dma(1), dma(1),
            dma(layers, tp), dma(layers, tp),
            dma(dp), dma(dp),
            dma(dp), dma(dp),
            dma(layers, dp), dma(layers, dp),
            dma(layers, tp // 2), dma(layers, tp // 2),
            dma(layers, tp // 2), dma(layers, tp // 2),
        ],
        compiler_params=pltpu.CompilerParams(collective_id=0, has_side_effects=True, vmem_limit_bytes=limit),
    )(
        stream, norm_gain, w_input, lam_re, lam_im, log_dt, turned_re, turned_im, readout_real,
        readout_imaginary, d_skip, w_val, w_gate,
        state.reshape(layers, rows_d * groups, lanes),
    )
    hbm_out = lambda a: jax.ShapeDtypeStruct(a.shape, a.dtype)
    out, states = pl.pallas_call(
        store,
        out_shape=(hbm_out(stream), jax.ShapeDtypeStruct((layers, rows_d * groups, lanes), F32)),
        in_specs=[vmem, vmem],
        out_specs=(hbm, hbm),
        scratch_shapes=[dma(3)],
    )(*(pltpu.with_memory_space_constraint(a, pltpu.VMEM) for a in (out, states)))
    return out, states.reshape(state.shape)


def solution(mesh):
    return jax.shard_map(
        functools.partial(per_device, mesh.shape["tp"], mesh.shape["dp"]),
        mesh=mesh,
        in_specs=(
            P("tp", "dp"),
            P(None, "dp"),
            P(None, "dp", "tp"),
            P(None, "tp", None),
            P(None, "tp", None),
            P(None, "tp"),
            P(None, "tp", None, None),
            P(None, "tp", None, None),
            P(None, "tp", None, None),
            P(None, "tp", None, None),
            P(None, "tp"),
            P(None, "tp", "dp"),
            P(None, "tp", "dp"),
            P(None, "dp", "tp", None),
        ),
        out_specs=(P("tp", "dp"), P(None, "dp", "tp", None)),
        check_vma=False,
    )
```

```python
import functools

import jax
import jax.numpy as jnp
from jax import lax
from jax.experimental import pallas as pl
from jax.experimental.pallas import tpu as pltpu
from jax.sharding import PartitionSpec as P

EPS = 1e-06
F32 = jnp.float32
BF16 = jnp.bfloat16
HIGHEST = lax.Precision.HIGHEST
NT = (((1,), (1,)), ((), ()))


def partner(me, k, n, back=False):
    if n & (n - 1):
        return (me + (n - k if back else k)) % n
    found, bit = 0, 1
    while bit < n:
        mine = (me // bit) % 2
        found = found + (bit * (1 - mine) if k & bit else bit * mine)
        bit *= 2
    return found


def kernel(
    tp, dp, chans,
    stream_hbm, gain_hbm, w_in_hbm, lam_re_hbm, lam_im_hbm, log_dt_hbm, b_re_hbm, b_im_hbm, c_re_hbm, c_im_hbm, skip_hbm,
    w_val_hbm, w_gate_hbm, state_hbm,
    out_ref, state,
    stream_ref, gain_ref, lam_re_ref, lam_im_ref, log_dt_ref, skip_ref,
    gains, w_in, w_wide, w_val, w_gate, b_re, b_im, c_re, c_im, drive, read,
    kept, proj, u_keep, masked, from_old, mix_w,
    x_own, x_all, x_wide, x_rest, part_send, part_recv, sq_send, sq_recv, mix_all, block, comb_send, comb_own, pair_recv, comb_recv,
    small_sem, load_sem, gain_ss, gain_rs, give_ss, give_rs, pass_ss, relay_ss, rest_ss, rest_rs, x_ss, x_rs, part_ss, part_rs, sq_ss, sq_rs, mix_ss, mix_rs, pair_ss, pair_rs, comb_ss, comb_rs,
):
    layers = b_re.shape[0]
    me_t, me_d = lax.axis_index("tp"), lax.axis_index("dp")
    rows_t, feats = stream_ref.shape
    rows_d, width = u_keep.shape[1:]
    per = rows_d // rows_t
    me_p, side = me_t // 2, me_t % 2
    groups, half = lam_re_ref.shape[1:]
    lanes = state.shape[2]
    sq_width = sq_send.shape[2]
    me_x, core, home = me_d // 2, me_d % 2, me_t // per
    mate = 2 * me_x + 1 - core
    halves, pairs, quads = dp // 2, per // 2, tp // 2
    spread = lambda block: block % 2 * halves + block // 2
    held = home % halves * 2 + home // halves
    final = held * per + me_t % per

    barrier = pltpu.get_barrier_semaphore()
    for k in range(1, dp):
        pl.semaphore_signal(barrier, inc=1, device_id={"dp": partner(me_d, k, dp)}, device_id_type=pl.DeviceIdType.MESH)
    for k in range(1, tp):
        pl.semaphore_signal(barrier, inc=1, device_id={"tp": partner(me_t, k, tp)}, device_id_type=pl.DeviceIdType.MESH)

    small = [
        pltpu.make_async_copy(src, dst, small_sem.at[i])
        for i, (src, dst) in enumerate(
            (
                (stream_hbm, stream_ref), (gain_hbm, gain_ref), (lam_re_hbm, lam_re_ref), (lam_im_hbm, lam_im_ref),
                (log_dt_hbm, log_dt_ref), (skip_hbm, skip_ref),
            )
        )
    ]
    for copy in small:
        copy.start()
    loads = {}
    for l in range(layers):
        for i, (src, dst) in enumerate(
            (
                (b_re_hbm, b_re), (b_im_hbm, b_im), (c_re_hbm, c_re), (c_im_hbm, c_im), (state_hbm, state),
                (w_in_hbm, w_in), (w_val_hbm, w_val), (w_gate_hbm, w_gate),
            )
        ):
            to = dst.at[l] if i != 5 else w_wide.at[l - 1, me_d] if l else w_in
            loads[l, i] = pltpu.make_async_copy(src.at[l], to, load_sem.at[l, i])
            loads[l, i].start()

    def send(src, dst, ss, rs, axis, to):
        return pltpu.make_async_remote_copy(
            src_ref=src, dst_ref=dst, send_sem=ss, recv_sem=rs, device_id={axis: to}, device_id_type=pl.DeviceIdType.MESH
        )

    def x_copy(l, k):
        to = partner(me_t, k, tp)
        if l == 0:
            return send(stream_ref, x_all.at[me_t], x_ss.at[l, to], x_rs.at[l, me_t], "tp", to)
        slot = me_t % per
        return pltpu.make_async_remote_copy(
            src_ref=x_own.at[l - 1], dst_ref=x_wide.at[l - 1, me_d, slot], send_sem=x_ss.at[l, to],
            recv_sem=x_rs.at[l, me_d * per + slot], device_id={"tp": to, "dp": held}, device_id_type=pl.DeviceIdType.MESH,
        )

    ends = quads - 1
    relay = (me_p == 1) | (me_p == ends - 1)
    origin = jnp.where(me_p == 1, ends, 0)

    def distant(to):
        return (jnp.abs(me_p - to // 2) == ends) & (ends > 2)

    def relay_copy(j):
        t = 2 * origin + j
        return send(x_all.at[t], x_all.at[t], relay_ss.at[j], x_rs.at[0, t], "tp", 2 * (ends - origin) + side)

    def rest_copy():
        return send(x_own.at[layers - 2], x_rest, rest_ss.at[0], rest_rs.at[0], "tp", final)

    def gain_copy(to):
        return send(gain_ref, gains.at[me_d], gain_ss.at[to], gain_rs.at[me_d], "dp", to)

    def give_copy(l, to):
        return send(w_in_hbm.at[l], w_wide.at[l - 1, me_d], give_ss.at[l - 1, to], give_rs.at[l - 1, me_d], "dp", to)

    def pass_copy(l, block):
        ref = w_wide.at[l - 1, block]
        return send(ref, ref, pass_ss.at[l - 1, block], give_rs.at[l - 1, block], "dp", mate)

    far = [2 * partner(me_x, k, dp // 2) + core for k in range(1, dp // 2)]

    def part_copy(to):
        return send(part_send.at[to], part_recv.at[me_d], part_ss.at[to], part_rs.at[me_d], "dp", to)

    def sq_copy(to):
        return send(sq_send.at[to], sq_recv.at[me_d], sq_ss.at[to], sq_rs.at[me_d], "dp", to)

    def mix_copy(l, to):
        return send(mix_all.at[l, me_d], mix_all.at[l, me_d], mix_ss.at[l, to], mix_rs.at[l, me_d], "dp", to)

    def comb_copy(l, r, to):
        return send(
            comb_send.at[l, 2 * r + side], comb_recv.at[l, me_p], comb_ss.at[l, to], comb_rs.at[l, me_p], "tp", 2 * to + side
        )

    def pair_copy(l, r):
        return send(
            comb_send.at[l, 2 * r + 1 - side], pair_recv.at[l, r], pair_ss.at[l, r], pair_rs.at[l, r], "tp", 2 * me_p + 1 - side
        )

    def arrival(ref, rs, axis):
        return send(ref, ref, rs, rs, axis, 0)

    lane_group = lax.broadcasted_iota(jnp.int32, (rows_d, width), 1) // chans
    eye = lax.broadcasted_iota(jnp.int32, (rows_d, sq_width), 0) == lax.broadcasted_iota(jnp.int32, (rows_d, sq_width), 1)

    group_eye = lax.broadcasted_iota(jnp.int32, (groups, groups), 0) == lax.broadcasted_iota(jnp.int32, (groups, groups), 1)

    def prepare(l):
        step_size = jnp.exp(jnp.sum(jnp.where(group_eye, log_dt_ref[l : l + 1, :], 0.0), axis=1, keepdims=True))
        lam_re, lam_im = lam_re_ref[l], lam_im_ref[l]
        decay = jnp.exp(lam_re * step_size)
        angle = lam_im * step_size
        keep_re = decay * jnp.cos(angle)
        keep_im = decay * jnp.sin(angle)
        denom = lam_re * lam_re + lam_im * lam_im
        ratio_re = ((keep_re - 1.0) * lam_re + keep_im * lam_im) / denom
        ratio_im = (keep_im * lam_re - (keep_re - 1.0) * lam_im) / denom
        keep_a = jnp.concatenate([keep_re, keep_re], axis=1)
        keep_b = jnp.concatenate([-keep_im, keep_im], axis=1)
        for i in range(5):
            loads[l, i].wait()
        for g in range(groups):
            t_re, t_im = b_re[l, g], b_im[l, g]
            r_re, r_im = ratio_re[g : g + 1, :], ratio_im[g : g + 1, :]
            drive[l, pl.ds(g * chans, chans), :] = jnp.concatenate(
                [r_re * t_re - r_im * t_im, r_re * t_im + r_im * t_re], axis=1
            )
        read[l] = jnp.concatenate([c_re[l].reshape(width, half), -c_im[l].reshape(width, half)], axis=1)
        for g in range(groups):
            old = state[l, pl.ds(g, rows_d, stride=groups), :]
            kept[l, pl.ds(g * rows_d, rows_d), :] = (
                keep_a[g : g + 1, :] * old + keep_b[g : g + 1, :] * pltpu.roll(old, lanes // 2, 1)
            )
        proj[...] = lax.dot_general(kept[l], read[l], NT, precision=HIGHEST, preferred_element_type=F32)
        total = jnp.zeros((rows_d, width), F32)
        for g in range(groups):
            total = jnp.where(lane_group == g, proj[pl.ds(g * rows_d, rows_d), :], total)
        from_old[l] = total
        full = lax.dot_general(drive[l], read[l], NT, precision=HIGHEST, preferred_element_type=F32)
        same = (
            lax.broadcasted_iota(jnp.int32, (width, width), 0) // chans
            == lax.broadcasted_iota(jnp.int32, (width, width), 1) // chans
        )
        mix_w[l] = jnp.where(same, full, 0.0)

    def update(l):
        u = u_keep[l]
        for g in range(groups):
            masked[pl.ds(g * rows_d, rows_d), :] = jnp.where(lane_group == g, u, 0.0)
        kept[l] = kept[l] + jnp.dot(masked[...], drive[l], precision=HIGHEST, preferred_element_type=F32)
        for g in range(groups):
            state[l, pl.ds(g, rows_d, stride=groups), :] = kept[l, pl.ds(g * rows_d, rows_d), :]

    small[0].wait()
    small[1].wait()
    pl.semaphore_wait(barrier, tp + dp - 2)
    for k in reversed(range(1, tp)):
        pl.when(jnp.logical_not(distant(partner(me_t, k, tp))))(lambda: x_copy(0, k).start())
    for k in range(1, dp):
        gain_copy(partner(me_d, k, dp)).start()
    x_all[me_t] = stream_ref[...]
    gains[me_d] = gain_ref[...]
    for copy in small[2:]:
        copy.wait()
    prepare(0)

    for l in range(layers):
        loads[l, 5].wait()
        if l == 0:
            gain = gain_ref[l : l + 1, :]
            own_part = own_sq = None
            if quads > 3:

                @pl.when(relay)
                def _():
                    for j in range(2):
                        arrival(x_all.at[2 * origin + j], x_rs.at[l, 2 * origin + j], "tp").wait_recv()
                        relay_copy(j).start()

            for k in reversed(range(dp)):
                to = partner(me_d, k, dp)
                for j in range(per):
                    t = to * per + j

                    @pl.when((t != me_t) & jnp.logical_not(relay & (t // 2 == origin) & (quads > 3)))
                    def _():
                        arrival(x_all.at[t], x_rs.at[l, t], "tp").wait_recv()

                x = x_all[pl.ds(to * per, per)].astype(F32).reshape(rows_d, feats)
                column = jnp.sum(x * x, axis=1, keepdims=True)
                squares = jnp.sum(jnp.where(eye, column, 0.0), axis=0, keepdims=True)
                product = jnp.dot((x * gain).astype(BF16), w_in[...], preferred_element_type=F32)
                if k:
                    sq_send[to] = jnp.broadcast_to(squares, (8, sq_width))
                    sq_copy(to).start()
                    part_send[to] = product.astype(BF16)
                    part_copy(to).start()
                else:
                    own_part, own_sq = product, squares
            for k in range(1, dp):
                by = partner(me_d, k, dp, True)
                arrival(sq_recv.at[by], sq_rs.at[by], "dp").wait_recv()
                own_sq = own_sq + sq_recv[by][0:1, :]
                arrival(part_recv.at[by], part_rs.at[by], "dp").wait_recv()
                own_part = own_part + part_recv[by].astype(F32)
            square_total = jnp.sum(jnp.where(eye, own_sq, 0.0), axis=1, keepdims=True)
        else:
            own_part = square_total = 0.0
            for k in range(dp):
                by = partner(me_d, k, dp, True)
                if k:
                    if l == 1:
                        arrival(gains.at[by], gain_rs.at[by], "dp").wait_recv()

                    @pl.when(by % 2 != core)
                    def _():
                        arrival(w_wide.at[l - 1, by], give_rs.at[l - 1, by], "dp").wait_recv()

                for j in range(per):

                    @pl.when((spread(me_d) * per + j != me_t) | (by != me_d))
                    def _():
                        arrival(x_wide.at[l - 1, by, j], x_rs.at[l, by * per + j], "tp").wait_recv()

                x = x_wide[l - 1, by].astype(F32).reshape(rows_d, feats)
                square_total = square_total + jnp.sum(x * x, axis=1, keepdims=True)
                normed = (x * gains[by, l : l + 1, :]).astype(BF16)
                own_part = own_part + jnp.dot(normed, w_wide[l - 1, by], preferred_element_type=F32)
        u = lax.rsqrt(square_total / (feats * dp) + EPS) * own_part
        u_keep[l] = u
        pre = from_old[l] + jnp.dot(u, mix_w[l], precision=HIGHEST, preferred_element_type=F32) + skip_ref[l : l + 1, :] * u
        mix_all[l, me_d] = jax.nn.gelu(pre).astype(BF16)
        for k in (*range(2, dp), 1) if l + 1 == layers else reversed(range(1, dp)):
            mix_copy(l, partner(me_d, k, dp)).start()
        if l + 1 == layers:
            pl.when(held != home)(lambda: rest_copy().start())
        loads[l, 6].wait()
        loads[l, 7].wait()

        def pass_on(by):
            for m in range(pairs):
                r = by * pairs + m
                q = (spread(by) if l + 1 < layers else by) * pairs + m
                arrival(pair_recv.at[l, r], pair_rs.at[l, r], "tp").wait_recv()
                total = block[2 * r + side] + pair_recv[l, r].astype(F32)

                @pl.when(q != me_p)
                def _():
                    comb_send[l, 2 * r + side] = total.astype(BF16)
                    comb_copy(l, r, q).start()

                @pl.when(q == me_p)
                def _():
                    comb_own[...] = total

        order = (0, 2, 1, *range(3, dp)) if l + 1 == layers else tuple(range(dp))
        for n, k in enumerate(order):
            by = partner(me_d, k, dp, True)
            if k:
                arrival(mix_all.at[l, by], mix_rs.at[l, by], "dp").wait_recv()
            mixed = mix_all[l, by]
            value = jnp.dot(mixed, w_val[l], preferred_element_type=F32)
            gate = jnp.dot(mixed, w_gate[l], preferred_element_type=F32)
            for j in range(per):
                rows = slice(j * rows_t, (j + 1) * rows_t)
                block[by * per + j, :, :feats] = value[rows]
                block[by * per + j, :, feats:] = gate[rows]
            for m in range(pairs):
                r = by * pairs + m
                comb_send[l, 2 * r + 1 - side] = block[2 * r + 1 - side].astype(BF16)
                pair_copy(l, r).start()
            if n > 1:
                pass_on(partner(me_d, order[n - 2], dp, True))
        if l + 1 < layers:
            for to in (*far, mate):
                give_copy(l + 1, to).start()
        for k in order[max(dp - 2, 0) :]:
            pass_on(partner(me_d, k, dp, True))

        if l + 1 == layers:
            update(l)
        if l + 1 < layers:
            prepare(l + 1)
        combined = comb_own[...]
        for k in range(1, tp // 2):
            by = partner(me_p, k, tp // 2, True)
            arrival(comb_recv.at[l, by], comb_rs.at[l, by], "tp").wait_recv()
            combined = combined + comb_recv[l, by].astype(F32)
        if l == 0:
            old = x_all[final]
        elif l + 1 < layers:
            old = x_own[l - 1]
        else:
            pl.when(held != home)(lambda: arrival(x_rest, rest_rs.at[0], "tp").wait_recv())
            old = x_rest[...]
        fresh = (old.astype(F32) + combined[:, :feats] * jax.nn.sigmoid(combined[:, feats:])).astype(BF16)
        if l + 1 < layers:
            x_own[l] = fresh
            for k in reversed(range(1, tp)):
                x_copy(l + 1, k).start()
            pl.when(held != me_d)(lambda: x_copy(l + 1, 0).start())

            @pl.when(held == me_d)
            def _():
                x_wide[l, me_d, me_t % per] = fresh

            if l + 2 == layers:

                @pl.when(held == home)
                def _():
                    x_rest[...] = fresh

            update(l)
            for owner in far:
                arrival(w_wide.at[l, owner], give_rs.at[l, owner], "dp").wait_recv()
                pass_copy(l + 1, owner).start()
        else:
            out_ref[...] = fresh

    for l in range(layers):
        for k in range(1, tp):
            gone = distant(partner(me_t, k, tp)) if l == 0 else False
            pl.when(jnp.logical_not(gone))(lambda: x_copy(l, k).wait_send())
        if l == 0 and quads > 3:

            @pl.when(relay)
            def _():
                for j in range(2):
                    relay_copy(j).wait_send()

        if l:
            pl.when(held != me_d)(lambda: x_copy(l, 0).wait_send())
            for to in (*far, mate):
                give_copy(l, to).wait_send()
            for owner in far:
                pass_copy(l, owner).wait_send()
        for k in range(1, tp // 2):
            comb_copy(l, 0, partner(me_p, k, tp // 2)).wait_send()
        for q in range(tp // 2):
            pair_copy(l, q).wait_send()
        for k in range(1, dp):
            mix_copy(l, partner(me_d, k, dp)).wait_send()
    pl.when(held != home)(lambda: rest_copy().wait_send())
    for k in range(1, dp):
        to = partner(me_d, k, dp)
        gain_copy(to).wait_send()
        part_copy(to).wait_send()
        sq_copy(to).wait_send()


def store(x_ref, state_ref, x_out, state_out, sem):
    middle = state_ref.shape[0] // 2
    first, second = pl.ds(0, middle), pl.ds(middle, state_ref.shape[0] - middle)
    copies = [
        pltpu.make_async_copy(state_ref.at[first], state_out.at[first], sem.at[0]),
        pltpu.make_async_copy(state_ref.at[second], state_out.at[second], sem.at[1]),
        pltpu.make_async_copy(x_ref, x_out, sem.at[2]),
    ]
    for copy in copies:
        copy.start()
    for copy in copies:
        copy.wait()


def per_device(
    tp, dp,
    stream, norm_gain, w_input, lam_re, lam_im, log_dt, b_re, b_im, readout_real, readout_imaginary, d_skip,
    w_val, w_gate, state,
):
    layers, feats, width = w_input.shape
    rows_t = stream.shape[0]
    rows_d, groups, lanes = state.shape[1:]
    chans = b_re.shape[-1]

    turned_re, turned_im = b_re.swapaxes(2, 3), b_im.swapaxes(2, 3)

    limit = 67043328 - 4 * layers * rows_d * groups * lanes - (256 << 10)
    vmem = pl.BlockSpec(memory_space=pltpu.VMEM)
    hbm = pl.BlockSpec(memory_space=pltpu.HBM)
    sq_width = max(rows_d, 128)
    dma = lambda *shape: pltpu.SemaphoreType.DMA(shape)
    out, states = pl.pallas_call(
        functools.partial(kernel, tp, dp, chans),
        out_shape=(pltpu.VMEM(stream.shape, BF16), pltpu.VMEM((layers, rows_d * groups, lanes), F32)),
        in_specs=[hbm] * 14,
        out_specs=(vmem, vmem),
        scratch_shapes=[
            pltpu.VMEM(stream.shape, BF16),
            *(pltpu.VMEM(a.shape, F32) for a in (norm_gain, lam_re, lam_im, log_dt, d_skip)),
            pltpu.VMEM((dp, layers, feats), F32),
            pltpu.VMEM((feats, width), BF16),
            pltpu.VMEM((layers - 1, dp, feats, width), BF16),
            pltpu.VMEM(w_val.shape, BF16),
            pltpu.VMEM(w_gate.shape, BF16),
            pltpu.VMEM(turned_re.shape, F32),
            pltpu.VMEM(turned_im.shape, F32),
            pltpu.VMEM(readout_real.shape, F32),
            pltpu.VMEM(readout_imaginary.shape, F32),
            pltpu.VMEM((layers, width, lanes), F32),
            pltpu.VMEM((layers, width, lanes), F32),
            pltpu.VMEM((layers, rows_d * groups, lanes), F32),
            pltpu.VMEM((rows_d * groups, width), F32),
            pltpu.VMEM((layers, rows_d, width), F32),
            pltpu.VMEM((rows_d * groups, width), F32),
            pltpu.VMEM((layers, rows_d, width), F32),
            pltpu.VMEM((layers, width, width), F32),
            pltpu.VMEM((layers - 1, rows_t, feats), BF16),
            pltpu.VMEM((tp, rows_t, feats), BF16),
            pltpu.VMEM((layers - 1, dp, rows_d // rows_t, rows_t, feats), BF16),
            pltpu.VMEM(stream.shape, BF16),
            pltpu.VMEM((dp, rows_d, width), BF16),
            pltpu.VMEM((dp, rows_d, width), BF16),
            pltpu.VMEM((dp, 8, sq_width), F32),
            pltpu.VMEM((dp, 8, sq_width), F32),
            pltpu.VMEM((layers, dp, rows_d, width), BF16),
            pltpu.VMEM((tp, rows_t, 2 * feats), F32),
            pltpu.VMEM((layers, tp, rows_t, 2 * feats), BF16),
            pltpu.VMEM((rows_t, 2 * feats), F32),
            pltpu.VMEM((layers, tp // 2, rows_t, 2 * feats), BF16),
            pltpu.VMEM((layers, tp // 2, rows_t, 2 * feats), BF16),
            dma(6),
            dma(layers, 8),
            dma(dp), dma(dp),
            dma(layers - 1, dp), dma(layers - 1, dp), dma(layers - 1, dp),
            dma(2), dma(1), dma(1),
            dma(layers, tp), dma(layers, tp),
            dma(dp), dma(dp),
            dma(dp), dma(dp),
            dma(layers, dp), dma(layers, dp),
            dma(layers, tp // 2), dma(layers, tp // 2),
            dma(layers, tp // 2), dma(layers, tp // 2),
        ],
        compiler_params=pltpu.CompilerParams(collective_id=0, has_side_effects=True, vmem_limit_bytes=limit),
    )(
        stream, norm_gain, w_input, lam_re, lam_im, log_dt, turned_re, turned_im, readout_real,
        readout_imaginary, d_skip, w_val, w_gate,
        state.reshape(layers, rows_d * groups, lanes),
    )
    hbm_out = lambda a: jax.ShapeDtypeStruct(a.shape, a.dtype)
    out, states = pl.pallas_call(
        store,
        out_shape=(hbm_out(stream), jax.ShapeDtypeStruct((layers, rows_d * groups, lanes), F32)),
        in_specs=[vmem, vmem],
        out_specs=(hbm, hbm),
        scratch_shapes=[dma(3)],
    )(*(pltpu.with_memory_space_constraint(a, pltpu.VMEM) for a in (out, states)))
    return out, states.reshape(state.shape)


def solution(mesh):
    return jax.shard_map(
        functools.partial(per_device, mesh.shape["tp"], mesh.shape["dp"]),
        mesh=mesh,
        in_specs=(
            P("tp", "dp"),
            P(None, "dp"),
            P(None, "dp", "tp"),
            P(None, "tp", None),
            P(None, "tp", None),
            P(None, "tp"),
            P(None, "tp", None, None),
            P(None, "tp", None, None),
            P(None, "tp", None, None),
            P(None, "tp", None, None),
            P(None, "tp"),
            P(None, "tp", "dp"),
            P(None, "tp", "dp"),
            P(None, "dp", "tp", None),
        ),
        out_specs=(P("tp", "dp"), P(None, "dp", "tp", None)),
        check_vma=False,
    )
```
